32 devices in a mesh: grp: 2 (over y), sp: 4 (over z), tp: 4 (over x, core).
Axes of the slice: x: 2, y: 2, z: 4, core: 2. Of those that a mesh axis runs over, the one named last changes fastest.
Arguments:
- latents: bfloat16 [3072, 4096], P(('grp', 'sp', 'tp')), parts along dimension 0, may hold values from -3 to 3
- conditions: float32 [4, 4096], P('grp', 'sp'), parts along dimension 0, may hold values from -6 to 6
- context: bfloat16 [1024, 4096], P(('grp', 'sp')), parts along dimension 0, may hold values from -6 to 6
- w_shift: bfloat16 [4096, 4096], P('sp', 'tp'), may hold values from -0.09375 to 0.09375
- w_scale: bfloat16 [4096, 4096], P('sp', 'tp'), may hold values from -0.09375 to 0.09375
- w_gate: bfloat16 [4096, 4096], P('sp', 'tp'), may hold values from -0.09375 to 0.09375
- w_qdown: bfloat16 [4096, 1024], P(None, 'tp'), may hold values from -2 to 2
- w_kvdown: bfloat16 [4096, 512], P(None, 'tp'), may hold values from -2 to 2
- w_rope: bfloat16 [4096, 32], replicated, may hold values from -0.09375 to 0.09375
- q_gain: float32 [1024], replicated, may hold values from 1 to 24
- latent_norm_gain: float32 [512], replicated, may hold values from 0.1 to 1.9
- query_up_weight: bfloat16 [1024, 3072], P(None, 'tp'), may hold values from -0.1875 to 0.1875
- key_up_weight: bfloat16 [512, 2048], P(None, 'tp'), may hold values from -0.25 to 0.25
- value_up_weight: bfloat16 [512, 2048], P(None, 'tp'), may hold values from -0.25 to 0.25
- context_bias: float32 [32], P('tp'), may hold values from 0.5 to 2
- w_out: bfloat16 [2048, 4096], P(None, 'tp'), may hold values from -0.5 to 0.5
Outputs:
- mixed: bfloat16 [3072, 4096], P(('grp', 'sp', 'tp')), parts along dimension 0
The draws below stay inside these ranges and needn't reach their ends.
There are 2 independent parts, one for each index of `grp`. The reference program is written for one: setup_inputs(seed, part) draws one part's arguments, and reference() takes and returns one part's arrays. A program takes and returns all parts, laid end to end along the dimension named above; an argument that names none is the same for every part. Nothing has to cross between parts.
All inputs are finite; a program needn't handle non-finite values.
Results may differ from the reference program's by a relative error of at most 0.01345.
The reference program's roundings to bfloat16 on the way count: a program that leaves them out, or rounds other values in their place, can miss the bound.
Values may be sent and summed in bfloat16 or wider, within the bound.
A program may use at most 64 MiB of HBM per device.

```python
import math
import jax
import jax.numpy as jnp
from jax import lax

MODEL_WIDTH = 4096
HEAD_TOTAL = 32
PLAIN_QK_DIM = 64
ROTARY_DIM = 32
VALUE_DIM = 64
QUERY_RANK = 1024
LATENT_KV_RANK = 512
GRID_W = 64
CTX = 512
TOKENS = 1536


def ascending_columns(key, row_count, col_count):
    entries = jax.random.normal(jax.random.fold_in(key, 11), (row_count, col_count), jnp.float32)
    jitter = jax.random.uniform(jax.random.fold_in(key, 12), (col_count,), jnp.float32, math.log(0.6), math.log(1.6))
    steepness = 10.0
    column_scale = jnp.exp(jitter + math.log(steepness) * jnp.arange(col_count, dtype=jnp.float32) / col_count)
    column_scale = column_scale / jnp.sqrt(jnp.mean(column_scale * column_scale))
    return jnp.clip(jnp.clip(entries, -4.0, 4.0) * column_scale * row_count ** (-0.5), -2.0, 2.0)


def draw_w_qdown(key, part):
    return ascending_columns(jax.random.fold_in(key, 3), MODEL_WIDTH, QUERY_RANK).astype(jnp.bfloat16)


def draw_w_kvdown(key, part):
    return ascending_columns(jax.random.fold_in(key, 5), MODEL_WIDTH, LATENT_KV_RANK).astype(jnp.bfloat16)


def draw_q_gain(key, part):
    return jax.random.uniform(jax.random.fold_in(key, 7), (QUERY_RANK,), jnp.float32, 1.5, 3.5)


def levels(stream_key, shape, shards, smallest, high):
    def one(position, shards_of):
        draws = jax.random.uniform(jax.random.fold_in(jax.random.fold_in(stream_key, 6), position), (shards_of,), jnp.float32, smallest / len(shards), high / len(shards))
        return jnp.repeat(jnp.exp(draws), shape[position] // shards_of).reshape((-1,) + (1,) * (len(shape) - position - 1))

    factor_of = one(*shards[0])
    for cut in shards[1:]:
        factor_of = factor_of * one(*cut)
    return factor_of


def noise(rng, extent, scale, most, cuts=(), held_as=jnp.bfloat16):
    loudness = levels(rng, extent, cuts, -0.22, 0.18) if cuts else 1.0
    result = jax.random.normal(rng, extent, jnp.float32) * scale * loudness
    return jnp.minimum(jnp.maximum(result, -most), most).astype(held_as)


def setup_inputs(seed: int = 0, part: int = 0) -> dict:
    streams_of = jax.random.split(jax.random.key(seed), 17)
    part_splits = jax.random.split(jax.random.fold_in(streams_of[16], part), 17)
    latents = noise(part_splits[0], (TOKENS, MODEL_WIDTH), 0.5, 3.0, ((0, 16),))
    conditions = noise(part_splits[1], (2, MODEL_WIDTH), 1.0, 6.0, ((1, 4),), jnp.float32)
    context = noise(part_splits[2], (CTX, MODEL_WIDTH), 1.0, 6.0, ((0, 4),))
    w_shift = noise(streams_of[3], (MODEL_WIDTH, MODEL_WIDTH), MODEL_WIDTH ** -0.5, 0.09375, ((0, 4), (1, 4)))
    w_scale = noise(streams_of[4], (MODEL_WIDTH, MODEL_WIDTH), MODEL_WIDTH ** -0.5, 0.09375, ((0, 4), (1, 4)))
    w_gate = noise(streams_of[5], (MODEL_WIDTH, MODEL_WIDTH), MODEL_WIDTH ** -0.5, 0.09375, ((0, 4), (1, 4)))
    w_qdown = draw_w_qdown(jax.random.fold_in(streams_of[16], 71), part)
    w_kvdown = draw_w_kvdown(jax.random.fold_in(streams_of[16], 71), part)
    w_rope = noise(streams_of[8], (MODEL_WIDTH, ROTARY_DIM), MODEL_WIDTH ** -0.5, 0.09375)
    q_gain = draw_q_gain(jax.random.fold_in(streams_of[16], 71), part)
    latent_norm_gain = jnp.clip(1.0 + 0.18 * jax.random.normal(streams_of[10], (LATENT_KV_RANK,), jnp.float32), 0.1, 1.9)
    query_up_weight = noise(streams_of[11], (QUERY_RANK, HEAD_TOTAL * (PLAIN_QK_DIM + ROTARY_DIM)), QUERY_RANK ** -0.5, 0.1875, ((1, 4),))
    key_up_weight = noise(streams_of[12], (LATENT_KV_RANK, HEAD_TOTAL * PLAIN_QK_DIM), LATENT_KV_RANK ** -0.5, 0.25, ((1, 4),))
    value_up_weight = noise(streams_of[13], (LATENT_KV_RANK, HEAD_TOTAL * VALUE_DIM), LATENT_KV_RANK ** -0.5, 0.25, ((1, 4),))
    context_bias = jnp.clip(0.5 + 1.5 * jax.random.uniform(streams_of[14], (HEAD_TOTAL,), jnp.float32) ** levels(streams_of[14], (HEAD_TOTAL,), ((0, 4),), -0.2, 0.2), 0.5, 2.0)
    w_out = noise(streams_of[15], (HEAD_TOTAL * VALUE_DIM, MODEL_WIDTH), (HEAD_TOTAL * VALUE_DIM // 16) ** -0.5, 0.5, ((1, 4),))
    return {"latents": latents, "conditions": conditions, "context": context, "w_shift": w_shift, "w_scale": w_scale, "w_gate": w_gate, "w_qdown": w_qdown, "w_kvdown": w_kvdown, "w_rope": w_rope, "q_gain": q_gain, "latent_norm_gain": latent_norm_gain, "query_up_weight": query_up_weight, "key_up_weight": key_up_weight, "value_up_weight": value_up_weight, "context_bias": context_bias, "w_out": w_out}


EPSILON = 1e-06

def layer_modulate(row_block, shift_by, scale_by):
    values = row_block.astype(jnp.float32)
    center = values - lax.optimization_barrier(jnp.mean(values, axis=-1, keepdims=True))
    spread = lax.optimization_barrier(jnp.mean(center * center, axis=-1, keepdims=True))
    normed = center * lax.rsqrt(spread + EPSILON)
    return (normed * (1.0 + scale_by) + shift_by).astype(jnp.bfloat16)

def rms_scale(raw_rows, gain_vec):
    values = raw_rows.astype(jnp.float32)
    factor = lax.rsqrt(lax.optimization_barrier(jnp.mean(values * values, axis=-1, keepdims=True)) + EPSILON)
    return (values * factor * gain_vec).astype(jnp.bfloat16)

def axial_turn(values, positions):
    freq_count = values.shape[-1] // 4
    inverse = 10000.0 ** (-jnp.arange(freq_count, dtype=jnp.float32) / freq_count)
    grid_row = (positions // GRID_W).astype(jnp.float32)
    grid_col = (positions % GRID_W).astype(jnp.float32)
    target = (positions.shape[0],) + (1,) * (values.ndim - 2) + (freq_count,)
    pieces = []
    for half_index, coordinate in enumerate((grid_row, grid_col)):
        angles = (coordinate[:, None] * inverse[None, :]).reshape(target)
        cosine = jnp.cos(angles)
        sine_of = jnp.sin(angles)
        segment = values[..., 2 * half_index * freq_count:2 * (half_index + 1) * freq_count]
        low_half = segment[..., :freq_count]
        high_half = segment[..., freq_count:]
        pieces.append(low_half * cosine - high_half * sine_of)
        pieces.append(low_half * sine_of + high_half * cosine)
    return jnp.concatenate(pieces, axis=-1)

def reference(latents, conditions, context, w_shift, w_scale, w_gate, w_qdown, w_kvdown, w_rope, q_gain, latent_norm_gain, query_up_weight, key_up_weight, value_up_weight, context_bias, w_out):
    cond_act = jax.nn.silu(conditions.astype(jnp.float32)).astype(jnp.bfloat16)
    shift_lat = jnp.dot(cond_act[0], w_shift, preferred_element_type=jnp.float32)
    scale_lat = jnp.dot(cond_act[0], w_scale, preferred_element_type=jnp.float32)
    gate_lat = jnp.dot(cond_act[0], w_gate, preferred_element_type=jnp.float32)
    shift_ctx = jnp.dot(cond_act[1], w_shift, preferred_element_type=jnp.float32)
    scale_ctx = jnp.dot(cond_act[1], w_scale, preferred_element_type=jnp.float32)
    h_lat = layer_modulate(latents, shift_lat, scale_lat)
    h_ctx = layer_modulate(context, shift_ctx, scale_ctx)
    cq_all = rms_scale(jnp.dot(h_lat, w_qdown, preferred_element_type=jnp.float32).astype(jnp.bfloat16), q_gain)
    ckv_lat = rms_scale(jnp.dot(h_lat, w_kvdown, preferred_element_type=jnp.float32).astype(jnp.bfloat16), latent_norm_gain)
    ckv_ctx = rms_scale(jnp.dot(h_ctx, w_kvdown, preferred_element_type=jnp.float32).astype(jnp.bfloat16), latent_norm_gain)
    positions = jnp.arange(TOKENS, dtype=jnp.int32)
    kr_lat = axial_turn(jnp.dot(h_lat, w_rope, preferred_element_type=jnp.float32), positions).astype(jnp.bfloat16)
    kr_ctx = jnp.dot(h_ctx, w_rope, preferred_element_type=jnp.float32).astype(jnp.bfloat16)
    q_all = jnp.dot(cq_all, query_up_weight, preferred_element_type=jnp.float32).reshape(TOKENS, HEAD_TOTAL, PLAIN_QK_DIM + ROTARY_DIM)
    queries = jnp.concatenate([q_all[..., :PLAIN_QK_DIM], axial_turn(q_all[..., PLAIN_QK_DIM:], positions)], axis=-1).astype(jnp.bfloat16)
    key_rows = jnp.concatenate([jnp.dot(ckv_lat, key_up_weight, preferred_element_type=jnp.float32).astype(jnp.bfloat16), jnp.dot(ckv_ctx, key_up_weight, preferred_element_type=jnp.float32).astype(jnp.bfloat16)], axis=0)
    value_rows = jnp.concatenate([jnp.dot(ckv_lat, value_up_weight, preferred_element_type=jnp.float32).astype(jnp.bfloat16), jnp.dot(ckv_ctx, value_up_weight, preferred_element_type=jnp.float32).astype(jnp.bfloat16)], axis=0)
    key_rows = key_rows.reshape(TOKENS + CTX, HEAD_TOTAL, PLAIN_QK_DIM)
    value_rows = value_rows.reshape(TOKENS + CTX, HEAD_TOTAL, VALUE_DIM)
    rope_keys = jnp.concatenate([kr_lat, kr_ctx], axis=0)
    is_ctx = (jnp.arange(TOKENS + CTX, dtype=jnp.int32) >= TOKENS).astype(jnp.float32)
    score_scale = (PLAIN_QK_DIM + ROTARY_DIM) ** (-0.5)

    def one_head(operands):
        head_q, head_k, head_v, head_bias = operands
        scores = jnp.dot(head_q[:, :PLAIN_QK_DIM], head_k.T, preferred_element_type=jnp.float32)
        scores = scores + jnp.dot(head_q[:, PLAIN_QK_DIM:], rope_keys.T, preferred_element_type=jnp.float32)
        scores = scores * score_scale + head_bias * is_ctx[None, :]
        largest = lax.optimization_barrier(jnp.max(scores, axis=-1, keepdims=True))
        exponent = jnp.exp(scores - largest)
        row_sum = lax.optimization_barrier(jnp.sum(exponent, axis=-1, keepdims=True))
        weights = exponent.astype(jnp.bfloat16)
        return (jnp.dot(weights, head_v, preferred_element_type=jnp.float32) / row_sum).astype(jnp.bfloat16)
    attended = lax.map(one_head, (queries.transpose(1, 0, 2), key_rows.transpose(1, 0, 2), value_rows.transpose(1, 0, 2), context_bias))
    attended = attended.transpose(1, 0, 2).reshape(TOKENS, HEAD_TOTAL * VALUE_DIM)
    projected = jnp.dot(attended, w_out, preferred_element_type=jnp.float32).astype(jnp.bfloat16)
    return (latents.astype(jnp.float32) + gate_lat * projected.astype(jnp.float32)).astype(jnp.bfloat16)
```

```python
import functools

import jax
import jax.numpy as jnp
import numpy as np
from jax import lax
from jax.experimental import pallas as pl
from jax.experimental.pallas import tpu as pltpu
from jax.sharding import PartitionSpec as P

PLAIN_QK_DIM = 64
ROTARY_DIM = 32
VALUE_DIM = 64
GRID_W = 64


EPSILON = 1e-06
NEGATIVE = -1e30


def layer_modulate(row_block, shift_by, scale_by):
    values = row_block.astype(jnp.float32)
    center = values - jnp.mean(values, axis=-1, keepdims=True)
    spread = jnp.mean(center * center, axis=-1, keepdims=True)
    normed = center * lax.rsqrt(spread + EPSILON)
    return (normed * (1.0 + scale_by) + shift_by).astype(jnp.bfloat16)


def rms_scale(raw_rows, gain_vec):
    values = raw_rows.astype(jnp.float32)
    factor = lax.rsqrt(jnp.mean(values * values, axis=-1, keepdims=True) + EPSILON)
    return (values * factor * gain_vec).astype(jnp.bfloat16)


def axial_turn(values, positions):
    freq_count = values.shape[-1] // 4
    inverse = 10000.0 ** (-jnp.arange(freq_count, dtype=jnp.float32) / freq_count)
    grid_row = (positions // GRID_W).astype(jnp.float32)
    grid_col = (positions % GRID_W).astype(jnp.float32)
    target = (positions.shape[0],) + (1,) * (values.ndim - 2) + (freq_count,)
    pieces = []
    for half_index, coordinate in enumerate((grid_row, grid_col)):
        angles = (coordinate[:, None] * inverse[None, :]).reshape(target)
        cosine = jnp.cos(angles)
        sine_of = jnp.sin(angles)
        segment = values[..., 2 * half_index * freq_count : 2 * (half_index + 1) * freq_count]
        low_half = segment[..., :freq_count]
        high_half = segment[..., freq_count:]
        pieces.append(low_half * cosine - high_half * sine_of)
        pieces.append(low_half * sine_of + high_half * cosine)
    return jnp.concatenate(pieces, axis=-1)


def plain_device(
    latents,
    conditions,
    context,
    w_shift,
    w_scale,
    w_gate,
    w_qdown,
    w_kvdown,
    w_rope,
    q_gain,
    latent_norm_gain,
    query_up_weight,
    key_up_weight,
    value_up_weight,
    context_bias,
    w_out,
):
    tp_count = lax.axis_size("tp")
    tp_index = lax.axis_index("tp")
    sp_index = lax.axis_index("sp")
    own_rows = latents.shape[0]
    tok_count = own_rows * tp_count
    ctx_share = context.shape[0] // tp_count
    cond_act = jax.nn.silu(conditions).astype(jnp.bfloat16)
    partial_mod = jnp.concatenate(
        [
            jnp.dot(cond_act, w_shift, preferred_element_type=jnp.float32),
            jnp.dot(cond_act, w_scale, preferred_element_type=jnp.float32),
            jnp.dot(cond_act[0:1], w_gate, preferred_element_type=jnp.float32),
        ],
        axis=0,
    )
    summed = lax.psum(partial_mod, "sp")
    modulation = lax.all_gather(summed, "tp", axis=1, tiled=True)
    ctx_own = lax.dynamic_slice_in_dim(context, tp_index * ctx_share, ctx_share, 0)
    h_lat = layer_modulate(latents, modulation[0], modulation[2])
    h_ctx = layer_modulate(ctx_own, modulation[1], modulation[3])
    h_own = jnp.concatenate([h_lat, h_ctx], axis=0)
    rope_raw = jnp.dot(h_own, w_rope, preferred_element_type=jnp.float32)
    own_pos = sp_index * tok_count + tp_index * own_rows + jnp.arange(own_rows, dtype=jnp.int32)
    kr_lat = axial_turn(rope_raw[:own_rows], own_pos).astype(jnp.bfloat16)
    kr_ctx = rope_raw[own_rows:].astype(jnp.bfloat16)
    arrived = lax.all_gather(h_own, "tp", axis=0, tiled=True)
    projected = jnp.concatenate(
        [
            jnp.dot(arrived, w_qdown, preferred_element_type=jnp.float32),
            jnp.dot(arrived, w_kvdown, preferred_element_type=jnp.float32),
        ],
        axis=1,
    ).astype(jnp.bfloat16)
    q_cols = w_qdown.shape[1]
    grouped = projected.reshape(tp_count, own_rows + ctx_share, projected.shape[1])
    cq_cols = grouped[:, :own_rows, :q_cols].reshape(tok_count, q_cols)
    kvl_cols = grouped[:, :own_rows, q_cols:].reshape(tok_count, w_kvdown.shape[1])
    kvc_cols = grouped[:, own_rows:, q_cols:].reshape(tp_count * ctx_share, w_kvdown.shape[1])
    cq_raw, kvl_raw, kvc_raw, krl_all, krc_all = (
        lax.all_gather(cq_cols, "tp", axis=1, tiled=True),
        lax.all_gather(kvl_cols, "tp", axis=1, tiled=True),
        lax.all_gather(kvc_cols, "tp", axis=1, tiled=True),
        lax.all_gather(kr_lat, "tp", axis=0, tiled=True),
        lax.all_gather(kr_ctx, "tp", axis=0, tiled=True),
    )
    cq_all = rms_scale(cq_raw, q_gain)
    ckv_all = jnp.concatenate(
        [rms_scale(kvl_raw, latent_norm_gain), rms_scale(kvc_raw, latent_norm_gain)], axis=0
    )
    kr_all = jnp.concatenate([krl_all, krc_all], axis=0)
    head_count = query_up_weight.shape[1] // (PLAIN_QK_DIM + ROTARY_DIM)
    q_all = jnp.dot(cq_all, query_up_weight, preferred_element_type=jnp.float32)
    q_all = q_all.reshape(tok_count, head_count, PLAIN_QK_DIM + ROTARY_DIM)
    query_pos = sp_index * tok_count + jnp.arange(tok_count, dtype=jnp.int32)
    queries = jnp.concatenate(
        [q_all[..., :PLAIN_QK_DIM], axial_turn(q_all[..., PLAIN_QK_DIM:], query_pos)], axis=-1
    ).astype(jnp.bfloat16)
    q_nope = queries[..., :PLAIN_QK_DIM]
    q_rope = queries[..., PLAIN_QK_DIM:]
    seg_rows = ckv_all.shape[0]
    is_ctx = (jnp.arange(seg_rows, dtype=jnp.int32) >= tok_count).astype(jnp.float32)
    bias_row = context_bias[None, :, None] * is_ctx[None, None, :]
    score_scale = (PLAIN_QK_DIM + ROTARY_DIM) ** (-0.5)

    def attend_block(running, key_block, value_block, rope_block):
        running_max, running_sum, numerator = running
        scores = jnp.einsum("ihd,jhd->ihj", q_nope, key_block, preferred_element_type=jnp.float32)
        scores = scores + jnp.einsum(
            "ihd,jd->ihj", q_rope, rope_block, preferred_element_type=jnp.float32
        )
        scores = scores * score_scale + bias_row
        new_max = jnp.maximum(running_max, jnp.max(scores, axis=-1))
        rescale = jnp.exp(running_max - new_max)
        exponent = jnp.exp(scores - new_max[..., None])
        running_sum = running_sum * rescale + jnp.sum(exponent, axis=-1)
        numerator = numerator * rescale[..., None] + jnp.einsum(
            "ihj,jhd->ihd",
            exponent.astype(jnp.bfloat16),
            value_block,
            preferred_element_type=jnp.float32,
        )
        return (new_max, running_sum, numerator)

    initial = (
        jnp.full((tok_count, head_count), NEGATIVE, jnp.float32),
        jnp.zeros((tok_count, head_count), jnp.float32),
        jnp.zeros((tok_count, head_count, VALUE_DIM), jnp.float32),
    )

    def expand_latent(key_group):
        latent_rows, rope_block = key_group
        key_block = jnp.dot(latent_rows, key_up_weight, preferred_element_type=jnp.float32).astype(
            jnp.bfloat16
        )
        value_block = jnp.dot(
            latent_rows, value_up_weight, preferred_element_type=jnp.float32
        ).astype(jnp.bfloat16)
        return (
            key_block.reshape(seg_rows, head_count, PLAIN_QK_DIM),
            value_block.reshape(seg_rows, head_count, VALUE_DIM),
            rope_block,
        )

    members = (
        lax.all_gather(ckv_all, "sp", axis=0, tiled=True),
        lax.all_gather(kr_all, "sp", axis=0, tiled=True),
    )
    block_count = members[0].shape[0] // seg_rows
    stacked = tuple(
        (member.reshape((block_count, seg_rows) + member.shape[1:]) for member in members)
    )

    def step_fn(state, key_group):
        key_block, value_block, rope_block = expand_latent(key_group)
        return (attend_block(state, key_block, value_block, rope_block), None)

    result, unused = lax.scan(step_fn, initial, stacked)
    running_max, running_sum, numerator = result
    attended = (
        (numerator / running_sum[..., None])
        .astype(jnp.bfloat16)
        .reshape(tok_count, head_count * VALUE_DIM)
    )
    proj_cols = jnp.dot(
        lax.all_gather(attended, "tp", axis=1, tiled=True),
        w_out,
        preferred_element_type=jnp.float32,
    )
    proj_rows = lax.all_to_all(
        proj_cols.astype(jnp.bfloat16), "tp", split_axis=0, concat_axis=1, tiled=True
    )
    mixed_rows = latents.astype(jnp.float32) + modulation[4] * proj_rows.astype(jnp.float32)
    return mixed_rows.astype(jnp.bfloat16)


MESH = pl.DeviceIdType.MESH
LOG2E = 1.4426950408889634
STEP = 16


def turn_tables(tokens):
    freq_count = ROTARY_DIM // 4
    inverse = 10000.0 ** (-np.arange(freq_count) / freq_count)
    position = np.arange(tokens)
    cosine = np.zeros((tokens, 128), np.float32)
    sine = np.zeros((tokens, 128), np.float32)
    cosine[:, :PLAIN_QK_DIM] = 1.0
    for half_index, coordinate in enumerate((position // GRID_W, position % GRID_W)):
        angles = coordinate[:, None] * inverse[None, :]
        low = PLAIN_QK_DIM + 2 * half_index * freq_count
        high = low + freq_count
        cosine[:, low : low + freq_count] = np.cos(angles)
        cosine[:, high : high + freq_count] = np.cos(angles)
        sine[:, low : low + freq_count] = -np.sin(angles)
        sine[:, high : high + freq_count] = np.sin(angles)
    return cosine, sine


def lanes_of(shape):
    return lax.broadcasted_iota(jnp.int32, shape, len(shape) - 1)


def turned(values, cosine, sine):
    lane = lanes_of(values.shape)
    swapped = jnp.where(
        (lane // 8) % 2 == 0, pltpu.roll(values, 120, 1), pltpu.roll(values, 8, 1)
    )
    return values * cosine + swapped * sine


def block_kernel(
    cond_ref,
    bias_ref,
    qgain_ref,
    kvgain_ref,
    rope_ref,
    lat_hbm,
    ctx_hbm,
    wsh_hbm,
    wsc_hbm,
    wga_hbm,
    wqd_hbm,
    wkd_hbm,
    wqu_hbm,
    wku_hbm,
    wvu_hbm,
    wo_hbm,
    cos_hbm,
    sin_hbm,
    out_ref,
    cond16,
    w3,
    lat,
    ctx,
    hid,
    wqd,
    wkvr,
    modp,
    mod,
    cq,
    kv,
    kvc,
    kraw,
    ck,
    cqn,
    wqu,
    wku,
    wvu,
    wo,
    cosv,
    sinv,
    qh,
    kb,
    vb,
    acc,
    mx,
    att,
    po,
    pr,
    load_sem,
    send_sem,
    recv_sem,
    zsend,
    zrecv,
    dsend,
    drecv,
):
    f32, bf16 = jnp.float32, jnp.bfloat16
    spn = lax.axis_size("sp")
    p = lax.axis_index("tp")
    z = lax.axis_index("sp")
    core = lax.rem(p, 2)
    side = p // 2
    p1, p2, p3 = p ^ 1, p ^ 2, p ^ 3
    own = lat.shape[1]
    width = lat.shape[2]
    tok = own * 4
    pair = own * 2
    ctxn = ctx.shape[0]
    seg = tok + ctxn
    modw = w3.shape[2]
    heads = qh.shape[0]
    hrow = seg // 2
    qcols = cq.shape[3]
    kcols = kv.shape[3]
    krank = 4 * kcols

    loads = []

    def load(src, dst):
        copy = pltpu.make_async_copy(src, dst, load_sem.at[len(loads)])
        loads.append(copy)
        copy.start()
        return copy

    l_lat = load(lat_hbm, lat.at[p])
    l_w3 = [load(ref, w3.at[i]) for i, ref in enumerate((wsh_hbm, wsc_hbm, wga_hbm))]
    l_ctx = load(ctx_hbm, ctx)
    l_kd = load(wkd_hbm, wkvr.at[:, pl.ds(0, kcols)])
    l_qd = load(wqd_hbm, wqd)
    table_rows = pl.ds(pl.multiple_of(z * tok, 8), tok)
    l_cos = load(cos_hbm.at[table_rows], cosv)
    l_sin = load(sin_hbm.at[table_rows], sinv)
    l_ku = load(wku_hbm, wku)
    l_vu = load(wvu_hbm, wvu)
    l_qu = load(wqu_hbm, wqu)
    l_wo = load(wo_hbm, wo)

    barrier = pltpu.get_barrier_semaphore()
    for peer in (p1, p2, p3):
        pl.semaphore_signal(barrier, inc=1, device_id={"tp": peer}, device_id_type=MESH)
    for d in range(1, spn):
        pl.semaphore_signal(
            barrier, inc=1, device_id={"sp": lax.rem(z + d, spn)}, device_id_type=MESH
        )

    sends = []

    def remote(src, dst, index, target):
        return pltpu.make_async_remote_copy(
            src_ref=src,
            dst_ref=dst,
            send_sem=send_sem.at[index],
            recv_sem=recv_sem.at[index],
            device_id=target,
            device_id_type=MESH,
        )

    def send(src, dst, index, target):
        copy = remote(src, dst, index, target)
        copy.start()
        sends.append(copy)
        return copy

    counter = [0]

    def fresh():
        counter[0] += 1
        return counter[0] - 1

    def spread(view, far_view=None):
        far_view = far_view or view
        i1, i2, i3 = fresh(), fresh(), fresh()
        first = send(view(p), view(p), i2, {"tp": p2})
        second = send(view(p), view(p), i1, {"tp": p1})

        def relay():
            first.wait_recv()
            third = send(far_view(p2), far_view(p2), i3, {"tp": p1})
            return third.wait_recv

        return relay, second.wait_recv

    cond16[...] = jnp.zeros_like(cond16)
    cond16[0:2, :] = cond_ref[...]
    conditions = cond16[...]
    act = (conditions / (1.0 + jnp.exp(-conditions))).astype(bf16)

    pl.semaphore_wait(barrier, 3 + spn - 1)
    l_lat.wait()
    half_own = own // 2
    relay_lat = []
    lat_near = []
    for piece in range(2):
        rows = pl.ds(piece * half_own, half_own)
        r, w = spread(lambda slot, rows=rows: lat.at[slot, rows])
        relay_lat.append(r)
        lat_near.append(w)

    for i in range(3):
        l_w3[i].wait()
        part = jnp.dot(act, w3[i], preferred_element_type=f32)
        modp[z, 2 * i : 2 * i + 2, :] = part[0:2]
    modp[z, 6:8, :] = jnp.zeros((2, modw), f32)
    mod_waits = []
    for d in range(1, spn):
        mod_waits.append(
            send(modp.at[z], modp.at[z], fresh(), {"sp": lax.rem(z + d, spn)})
        )
    wkvr[:, kcols:] = jnp.zeros((width, wkvr.shape[1] - kcols), bf16)
    wkvr[:, kcols : kcols + ROTARY_DIM] = rope_ref[...]
    for copy in mod_waits:
        copy.wait_recv()
    total = modp[0]
    for i in range(1, spn):
        total = total + modp[i]
    mod[p] = total
    mod_waits = [send(mod.at[p], mod.at[p], fresh(), {"tp": peer}) for peer in (p2, p3, p1)]
    lat_far = [relay_lat[0]()]
    for copy in mod_waits:
        copy.wait_recv()

    def modulate(src, row_count, dst_row, which):
        @pl.loop(0, row_count // STEP)
        def _(i):
            rows = pl.ds(pl.multiple_of(i * STEP, STEP), STEP)
            values = src[rows, :].astype(f32)
            center = values - jnp.mean(values, axis=-1, keepdims=True)
            spread_of = jnp.mean(center * center, axis=-1, keepdims=True)
            normed = center * lax.rsqrt(spread_of + EPSILON)
            to = pl.ds(pl.multiple_of(dst_row + i * STEP, STEP), STEP)
            for j in range(4):
                shift_by = mod[j, which : which + 1, :]
                scale_by = mod[j, 2 + which : 3 + which, :]
                cols = slice(j * modw, (j + 1) * modw)
                hid[to, cols] = (normed[:, cols] * (1.0 + scale_by) + shift_by).astype(bf16)

    l_ctx.wait()
    modulate(ctx, ctxn, tok, 1)
    l_kd.wait()
    l_qd.wait()
    mixed_ctx = jnp.dot(hid[tok:, :], wkvr[...], preferred_element_type=f32)
    kvc[p] = mixed_ctx[:, :kcols].astype(bf16)
    kraw[tok:, :] = mixed_ctx[:, kcols:]
    relays = [spread(lambda slot: kvc.at[slot])]

    modulate(lat.at[p], own, p * own, 0)
    for w in lat_near:
        w()
    modulate(lat.at[p1], own, p1 * own, 0)

    def down(half):
        rows = pl.ds(pl.multiple_of(half * pair, STEP), pair)
        both = jnp.dot(hid[rows, :], wkvr[...], preferred_element_type=f32)
        kv[p, half] = both[:, :kcols].astype(bf16)
        kraw[rows, :] = both[:, kcols:]
        one = spread(lambda slot: kv.at[slot, half], lambda slot: kv.at[slot, 1 - half])
        cq[p, half] = jnp.dot(hid[rows, :], wqd[...], preferred_element_type=f32).astype(bf16)
        return one, spread(lambda slot: cq.at[slot, half], lambda slot: cq.at[slot, 1 - half])

    kv_a, cq_a = down(side)
    lat_far.append(relay_lat[1]())
    modulate(lat.at[p2], own, p2 * own, 0)
    for w in lat_far:
        w()
    modulate(lat.at[p3], own, p3 * own, 0)
    kv_b, cq_b = down(1 - side)
    relays += [kv_a, kv_b]
    far = [r() for r, _ in relays]
    for w in far:
        w()
    for _, near in relays:
        near()

    l_cos.wait()
    l_sin.wait()
    kr_lat = turned(pltpu.roll(kraw[:tok, :], 64, 1), cosv[...], sinv[...])
    kraw[:tok, :] = kr_lat
    kraw[tok:, :] = pltpu.roll(kraw[tok:, :], 64, 1)
    for hf in range(2):
        for t in range(4):
            packed = None
            for j in range(4):
                first_row = hf * hrow + (4 * t + j) * STEP
                moved = pltpu.roll(
                    kraw[first_row : first_row + STEP, :], (32 * j + 64) % 128, 1
                )
                packed = moved if packed is None else packed + moved
            ck[z, hf, hrow : hrow + STEP, 128 * t : 128 * t + 128] = packed.astype(bf16)

    def rms(pieces, gain_ref, store):
        values = [piece.astype(f32) for piece in pieces]
        total_of = None
        for v in values:
            s = jnp.sum(v * v, axis=-1, keepdims=True)
            total_of = s if total_of is None else total_of + s
        cols = values[0].shape[1]
        factor = lax.rsqrt(total_of / (cols * len(values)) + EPSILON)
        for j, v in enumerate(values):
            gain = gain_ref[0:1, j * cols : (j + 1) * cols]
            store(slice(j * cols, (j + 1) * cols), (v * factor * gain).astype(bf16))

    for piece in range(seg // 64):
        base = piece * 64
        if base < tok:
            chunk = [kv[r, base // pair, base % pair : base % pair + 64, :] for r in range(4)]
        else:
            chunk = [kvc[r, base - tok : base - tok + 64, :] for r in range(4)]

        def put(cols, value, base=base):
            ck[z, base // hrow, base % hrow : base % hrow + 64, cols] = value

        rms(chunk, kvgain_ref, put)

    def hop(origin, target, way):
        return pltpu.make_async_remote_copy(
            src_ref=ck.at[origin, core],
            dst_ref=ck.at[origin, core],
            send_sem=zsend.at[way, origin],
            recv_sem=zrecv.at[origin],
            device_id={"sp": target},
            device_id_type=MESH,
        )

    def cross(origin, half):
        return pltpu.make_async_remote_copy(
            src_ref=ck.at[origin, half],
            dst_ref=ck.at[origin, half],
            send_sem=dsend.at[origin],
            recv_sem=drecv.at[origin],
            device_id={"tp": p1},
            device_id_type=MESH,
        )

    has_right = z + 1 < spn
    has_left = z >= 1

    @pl.when(has_right)
    def _():
        hop(z, z + 1, 0).start()

    @pl.when(has_left)
    def _():
        hop(z, z - 1, 1).start()

    w_cq = [cq_a[0](), cq_b[0]()]
    for w in w_cq:
        w()
    cq_a[1]()
    cq_b[1]()
    for piece in range(tok // 64):
        base = piece * 64
        chunk = [cq[r, base // pair, base % pair : base % pair + 64, :] for r in range(4)]

        def put(cols, value, base=base):
            cqn[base : base + 64, cols] = value

        rms(chunk, qgain_ref, put)
    l_qu.wait()
    q_all = jnp.dot(cqn[...], wqu[...], preferred_element_type=f32)
    lane = lanes_of((tok, 128))
    for h in range(heads):
        offset = h * (PLAIN_QK_DIM + ROTARY_DIM)
        tile, shift = offset // 128, offset % 128
        head = q_all[:, 128 * tile : 128 * tile + 128]
        if shift:
            head = pltpu.roll(head, 128 - shift, 1)
            if shift + PLAIN_QK_DIM + ROTARY_DIM > 128:
                rest = pltpu.roll(q_all[:, 128 * tile + 128 : 128 * tile + 256], 128 - shift, 1)
                head = jnp.where(lane < 128 - shift, head, rest)
        qh[h] = turned(head, cosv[...], sinv[...]).astype(bf16)
    l_ku.wait()
    l_vu.wait()
    acc[...] = jnp.zeros_like(acc)
    mx[...] = jnp.full(mx.shape, NEGATIVE, f32)
    factor = (PLAIN_QK_DIM + ROTARY_DIM) ** (-0.5) * LOG2E

    def arrive(step):
        left, right = z - 1 - step, z + 1 + step

        @pl.when(left >= 0)
        def _():
            hop(left, z, 0).wait_recv()
            cross(left, core).start()

            @pl.when(has_right)
            def _():
                hop(left, z + 1, 0).start()

        @pl.when(right < spn)
        def _():
            hop(right, z, 1).wait_recv()
            cross(right, core).start()

            @pl.when(has_left)
            def _():
                hop(right, z - 1, 1).start()

    def expand(block):
        lane_h = lanes_of((hrow, 128))
        ones = (lane_h == VALUE_DIM).astype(f32)
        lane_s = lanes_of((STEP, 128))
        on_rope = (lane_s >= PLAIN_QK_DIM) & (lane_s < PLAIN_QK_DIM + ROTARY_DIM)
        for hf in range(2):
            rows = slice(hf * hrow, (hf + 1) * hrow)
            latent_rows = ck[block, hf, :hrow, :]
            pieces = []
            for t in range(4):
                packed = ck[block, hf, hrow : hrow + STEP, 128 * t : 128 * t + 128].astype(f32)
                for j in range(4):
                    moved = pltpu.roll(packed, (192 - 32 * j) % 128, 1)
                    pieces.append(jnp.where(on_rope, moved, 0.0))
            rope_key = jnp.concatenate(pieces, axis=0)
            keys = jnp.dot(latent_rows, wku[...], preferred_element_type=f32)
            vals = jnp.dot(latent_rows, wvu[...], preferred_element_type=f32)
            for hp in range(heads // 2):
                cols = slice(128 * hp, 128 * hp + 128)
                k2, v2 = keys[:, cols], vals[:, cols]
                kb[2 * hp, rows, :] = jnp.where(lane_h < 64, k2, rope_key).astype(bf16)
                kb[2 * hp + 1, rows, :] = jnp.where(
                    lane_h < 64, pltpu.roll(k2, 64, 1), rope_key
                ).astype(bf16)
                vb[2 * hp, rows, :] = jnp.where(lane_h < 64, v2, ones).astype(bf16)
                vb[2 * hp + 1, rows, :] = jnp.where(
                    lane_h < 64, pltpu.roll(v2, 64, 1), ones
                ).astype(bf16)

    def attend(h):
        scores = lax.dot_general(
            qh[h], kb[h], (((1,), (1,)), ((), ())), preferred_element_type=f32
        )
        lat_s = scores[:, :tok] * factor
        ctx_s = scores[:, tok:] * factor + bias_ref[h] * LOG2E
        old = mx[h]
        best = jnp.maximum(
            jnp.max(lat_s, axis=-1, keepdims=True), jnp.max(ctx_s, axis=-1, keepdims=True)
        )
        new = jnp.maximum(old, best)
        mx[h] = new
        top = new[:, 0:1]
        weights = jnp.concatenate([jnp.exp2(lat_s - top), jnp.exp2(ctx_s - top)], axis=1)
        acc[h] = acc[h] * jnp.exp2(old - new) + jnp.dot(
            weights.astype(bf16), vb[h], preferred_element_type=f32
        )

    def block_at(step):
        below = jnp.minimum(z, spn - 1 - z)
        near = jnp.where(lax.rem(step, 2) == 1, z - (step + 1) // 2, z + step // 2)
        past = jnp.where(z < spn - 1 - z, step, spn - 1 - step)
        return jnp.where(step <= 2 * below, near, past)

    @pl.loop(0, spn)
    def _(step):
        @pl.when(step > 0)
        def _():
            arrive(step - 1)

        block = block_at(step)

        @pl.when(step > 0)
        def _():
            cross(block, 1 - core).wait_recv()

        expand(block)
        for h in range(heads):
            attend(h)

    att_relays = []
    lane64 = lane < 64
    for hp in range(heads // 2):
        outs = []
        for h in (2 * hp, 2 * hp + 1):
            a = acc[h]
            outs.append(a / a[:, VALUE_DIM : VALUE_DIM + 1])
        att[p, hp] = jnp.where(lane64, outs[0], pltpu.roll(outs[1], 64, 1)).astype(bf16)
        att_relays.append(spread(lambda slot, hp=hp: att.at[slot, hp]))
    att_far = [r() for r, _ in att_relays]
    for w in att_far:
        w()
    for _, near in att_relays:
        near()
    l_wo.wait()
    final = []
    for dest in (p2, p3, p1, p):
        rows = pl.ds(pl.multiple_of(dest * own, STEP), own)
        joined = jnp.concatenate(
            [att[r, hp, rows, :] for r in range(4) for hp in range(heads // 2)], axis=1
        )
        made = jnp.dot(joined, wo[...], preferred_element_type=f32).astype(bf16)
        if dest is p:
            pr[p] = made
        else:
            po[dest] = made
            final.append(send(po.at[dest], pr.at[p], fresh(), {"tp": dest}))
    for copy in final:
        copy.wait_recv()

    @pl.loop(0, own // STEP)
    def _(i):
        rows = pl.ds(pl.multiple_of(i * STEP, STEP), STEP)
        for j in range(4):
            cols = slice(j * modw, (j + 1) * modw)
            gate = mod[j, 4:5, :]
            out_ref[rows, cols] = (
                lat[p, rows, cols].astype(f32) + gate * pr[j, rows, :].astype(f32)
            ).astype(bf16)

    for copy in sends:
        copy.wait_send()

    @pl.when(has_right)
    def _():
        hop(z, z + 1, 0).wait_send()

    @pl.when(has_left)
    def _():
        hop(z, z - 1, 1).wait_send()

    for step in range(spn - 1):
        left, right = z - 1 - step, z + 1 + step

        @pl.when(left >= 0)
        def _():
            cross(left, core).wait_send()

            @pl.when(has_right)
            def _():
                hop(left, z + 1, 0).wait_send()

        @pl.when(right < spn)
        def _():
            cross(right, core).wait_send()

            @pl.when(has_left)
            def _():
                hop(right, z - 1, 1).wait_send()


def fused_device(
    latents,
    conditions,
    context,
    w_shift,
    w_scale,
    w_gate,
    w_qdown,
    w_kvdown,
    w_rope,
    q_gain,
    latent_norm_gain,
    query_up_weight,
    key_up_weight,
    value_up_weight,
    context_bias,
    w_out,
):
    f32, bf16 = jnp.float32, jnp.bfloat16
    spn = lax.axis_size("sp")
    own, width = latents.shape
    ctxn = context.shape[0]
    tok = 4 * own
    seg = tok + ctxn
    heads = context_bias.shape[0]
    modw = w_shift.shape[1]
    kdim, qcols = w_qdown.shape
    kcols = w_kvdown.shape[1]
    cosine, sine = turn_tables(tok * spn)
    vmem = pl.BlockSpec(memory_space=pltpu.VMEM)
    smem = pl.BlockSpec(memory_space=pltpu.SMEM)
    hbm = pl.BlockSpec(memory_space=pl.ANY)
    V, DMA = pltpu.VMEM, pltpu.SemaphoreType.DMA
    scratch = [
        V((16, conditions.shape[1]), f32),
        V((3,) + w_shift.shape, bf16),
        V((4, own, width), bf16),
        V((ctxn, width), bf16),
        V((seg, width), bf16),
        V((kdim, qcols), bf16),
        V((kdim, kcols + 128), bf16),
        V((spn, 8, modw), f32),
        V((4, 8, modw), f32),
        V((4, 2, 2 * own, qcols), bf16),
        V((4, 2, 2 * own, kcols), bf16),
        V((4, ctxn, kcols), bf16),
        V((seg, 128), f32),
        V((spn, 2, seg // 2 + STEP, 4 * kcols), bf16),
        V((tok, 4 * qcols), bf16),
        V(query_up_weight.shape, bf16),
        V(key_up_weight.shape, bf16),
        V(value_up_weight.shape, bf16),
        V(w_out.shape, bf16),
        V((tok, 128), f32),
        V((tok, 128), f32),
        V((heads, tok, 128), bf16),
        V((heads, seg, 128), bf16),
        V((heads, seg, 128), bf16),
        V((heads, tok, 128), f32),
        V((heads, tok, 128), f32),
        V((4, heads // 2, tok, 128), bf16),
        V((4, own, modw), bf16),
        V((4, own, modw), bf16),
        DMA((13,)),
        DMA((48,)),
        DMA((48,)),
        DMA((2, spn)),
        DMA((spn,)),
        DMA((spn,)),
        DMA((spn,)),
    ]
    return pl.pallas_call(
        block_kernel,
        out_shape=jax.ShapeDtypeStruct(latents.shape, bf16),
        in_specs=[vmem, smem, vmem, vmem, vmem] + [hbm] * 13,
        out_specs=vmem,
        scratch_shapes=scratch,
        compiler_params=pltpu.CompilerParams(
            collective_id=0, has_side_effects=True, vmem_limit_bytes=60 * 1024 * 1024
        ),
    )(
        conditions,
        context_bias,
        q_gain[None, :],
        latent_norm_gain[None, :],
        w_rope,
        latents,
        context,
        w_shift,
        w_scale,
        w_gate,
        w_qdown,
        w_kvdown,
        query_up_weight,
        key_up_weight,
        value_up_weight,
        w_out,
        jnp.asarray(cosine),
        jnp.asarray(sine),
    )


def on_device(*arrays):
    latents, context, bias = arrays[0], arrays[2], arrays[14]
    fits = (
        lax.axis_size("tp") == 4
        and latents.shape[0] % 32 == 0
        and context.shape[0] % 64 == 0
        and (4 * latents.shape[0] + context.shape[0]) == 512
        and arrays[6].shape[1] == 256
        and arrays[7].shape[1] == 128
        and bias.shape[0] == 8
    )
    return fused_device(*arrays) if fits else plain_device(*arrays)


def solution(mesh):
    in_specs = (
        P(("grp", "sp", "tp"), None),
        P("grp", "sp"),
        P(("grp", "sp"), None),
        P("sp", "tp"),
        P("sp", "tp"),
        P("sp", "tp"),
        P(None, "tp"),
        P(None, "tp"),
        P(),
        P(),
        P(),
        P(None, "tp"),
        P(None, "tp"),
        P(None, "tp"),
        P("tp"),
        P(None, "tp"),
    )
    out_specs = P(("grp", "sp", "tp"), None)
    return jax.shard_map(
        on_device, mesh=mesh, in_specs=in_specs, out_specs=out_specs, check_vma=False
    )
```

```python
import functools

import jax
import jax.numpy as jnp
import numpy as np
from jax import lax
from jax.experimental import pallas as pl
from jax.experimental.pallas import tpu as pltpu
from jax.sharding import PartitionSpec as P

PLAIN_QK_DIM = 64
ROTARY_DIM = 32
VALUE_DIM = 64
GRID_W = 64


EPSILON = 1e-06
NEGATIVE = -1e30


def layer_modulate(row_block, shift_by, scale_by):
    values = row_block.astype(jnp.float32)
    center = values - jnp.mean(values, axis=-1, keepdims=True)
    spread = jnp.mean(center * center, axis=-1, keepdims=True)
    normed = center * lax.rsqrt(spread + EPSILON)
    return (normed * (1.0 + scale_by) + shift_by).astype(jnp.bfloat16)


def rms_scale(raw_rows, gain_vec):
    values = raw_rows.astype(jnp.float32)
    factor = lax.rsqrt(jnp.mean(values * values, axis=-1, keepdims=True) + EPSILON)
    return (values * factor * gain_vec).astype(jnp.bfloat16)


def axial_turn(values, positions):
    freq_count = values.shape[-1] // 4
    inverse = 10000.0 ** (-jnp.arange(freq_count, dtype=jnp.float32) / freq_count)
    grid_row = (positions // GRID_W).astype(jnp.float32)
    grid_col = (positions % GRID_W).astype(jnp.float32)
    target = (positions.shape[0],) + (1,) * (values.ndim - 2) + (freq_count,)
    pieces = []
    for half_index, coordinate in enumerate((grid_row, grid_col)):
        angles = (coordinate[:, None] * inverse[None, :]).reshape(target)
        cosine = jnp.cos(angles)
        sine_of = jnp.sin(angles)
        segment = values[..., 2 * half_index * freq_count : 2 * (half_index + 1) * freq_count]
        low_half = segment[..., :freq_count]
        high_half = segment[..., freq_count:]
        pieces.append(low_half * cosine - high_half * sine_of)
        pieces.append(low_half * sine_of + high_half * cosine)
    return jnp.concatenate(pieces, axis=-1)


def plain_device(
    latents,
    conditions,
    context,
    w_shift,
    w_scale,
    w_gate,
    w_qdown,
    w_kvdown,
    w_rope,
    q_gain,
    latent_norm_gain,
    query_up_weight,
    key_up_weight,
    value_up_weight,
    context_bias,
    w_out,
):
    tp_count = lax.axis_size("tp")
    tp_index = lax.axis_index("tp")
    sp_index = lax.axis_index("sp")
    own_rows = latents.shape[0]
    tok_count = own_rows * tp_count
    ctx_share = context.shape[0] // tp_count
    cond_act = jax.nn.silu(conditions).astype(jnp.bfloat16)
    partial_mod = jnp.concatenate(
        [
            jnp.dot(cond_act, w_shift, preferred_element_type=jnp.float32),
            jnp.dot(cond_act, w_scale, preferred_element_type=jnp.float32),
            jnp.dot(cond_act[0:1], w_gate, preferred_element_type=jnp.float32),
        ],
        axis=0,
    )
    summed = lax.psum(partial_mod, "sp")
    modulation = lax.all_gather(summed, "tp", axis=1, tiled=True)
    ctx_own = lax.dynamic_slice_in_dim(context, tp_index * ctx_share, ctx_share, 0)
    h_lat = layer_modulate(latents, modulation[0], modulation[2])
    h_ctx = layer_modulate(ctx_own, modulation[1], modulation[3])
    h_own = jnp.concatenate([h_lat, h_ctx], axis=0)
    rope_raw = jnp.dot(h_own, w_rope, preferred_element_type=jnp.float32)
    own_pos = sp_index * tok_count + tp_index * own_rows + jnp.arange(own_rows, dtype=jnp.int32)
    kr_lat = axial_turn(rope_raw[:own_rows], own_pos).astype(jnp.bfloat16)
    kr_ctx = rope_raw[own_rows:].astype(jnp.bfloat16)
    arrived = lax.all_gather(h_own, "tp", axis=0, tiled=True)
    projected = jnp.concatenate(
        [
            jnp.dot(arrived, w_qdown, preferred_element_type=jnp.float32),
            jnp.dot(arrived, w_kvdown, preferred_element_type=jnp.float32),
        ],
        axis=1,
    ).astype(jnp.bfloat16)
    q_cols = w_qdown.shape[1]
    grouped = projected.reshape(tp_count, own_rows + ctx_share, projected.shape[1])
    cq_cols = grouped[:, :own_rows, :q_cols].reshape(tok_count, q_cols)
    kvl_cols = grouped[:, :own_rows, q_cols:].reshape(tok_count, w_kvdown.shape[1])
    kvc_cols = grouped[:, own_rows:, q_cols:].reshape(tp_count * ctx_share, w_kvdown.shape[1])
    cq_raw, kvl_raw, kvc_raw, krl_all, krc_all = (
        lax.all_gather(cq_cols, "tp", axis=1, tiled=True),
        lax.all_gather(kvl_cols, "tp", axis=1, tiled=True),
        lax.all_gather(kvc_cols, "tp", axis=1, tiled=True),
        lax.all_gather(kr_lat, "tp", axis=0, tiled=True),
        lax.all_gather(kr_ctx, "tp", axis=0, tiled=True),
    )
    cq_all = rms_scale(cq_raw, q_gain)
    ckv_all = jnp.concatenate(
        [rms_scale(kvl_raw, latent_norm_gain), rms_scale(kvc_raw, latent_norm_gain)], axis=0
    )
    kr_all = jnp.concatenate([krl_all, krc_all], axis=0)
    head_count = query_up_weight.shape[1] // (PLAIN_QK_DIM + ROTARY_DIM)
    q_all = jnp.dot(cq_all, query_up_weight, preferred_element_type=jnp.float32)
    q_all = q_all.reshape(tok_count, head_count, PLAIN_QK_DIM + ROTARY_DIM)
    query_pos = sp_index * tok_count + jnp.arange(tok_count, dtype=jnp.int32)
    queries = jnp.concatenate(
        [q_all[..., :PLAIN_QK_DIM], axial_turn(q_all[..., PLAIN_QK_DIM:], query_pos)], axis=-1
    ).astype(jnp.bfloat16)
    q_nope = queries[..., :PLAIN_QK_DIM]
    q_rope = queries[..., PLAIN_QK_DIM:]
    seg_rows = ckv_all.shape[0]
    is_ctx = (jnp.arange(seg_rows, dtype=jnp.int32) >= tok_count).astype(jnp.float32)
    bias_row = context_bias[None, :, None] * is_ctx[None, None, :]
    score_scale = (PLAIN_QK_DIM + ROTARY_DIM) ** (-0.5)

    def attend_block(running, key_block, value_block, rope_block):
        running_max, running_sum, numerator = running
        scores = jnp.einsum("ihd,jhd->ihj", q_nope, key_block, preferred_element_type=jnp.float32)
        scores = scores + jnp.einsum(
            "ihd,jd->ihj", q_rope, rope_block, preferred_element_type=jnp.float32
        )
        scores = scores * score_scale + bias_row
        new_max = jnp.maximum(running_max, jnp.max(scores, axis=-1))
        rescale = jnp.exp(running_max - new_max)
        exponent = jnp.exp(scores - new_max[..., None])
        running_sum = running_sum * rescale + jnp.sum(exponent, axis=-1)
        numerator = numerator * rescale[..., None] + jnp.einsum(
            "ihj,jhd->ihd",
            exponent.astype(jnp.bfloat16),
            value_block,
            preferred_element_type=jnp.float32,
        )
        return (new_max, running_sum, numerator)

    initial = (
        jnp.full((tok_count, head_count), NEGATIVE, jnp.float32),
        jnp.zeros((tok_count, head_count), jnp.float32),
        jnp.zeros((tok_count, head_count, VALUE_DIM), jnp.float32),
    )

    def expand_latent(key_group):
        latent_rows, rope_block = key_group
        key_block = jnp.dot(latent_rows, key_up_weight, preferred_element_type=jnp.float32).astype(
            jnp.bfloat16
        )
        value_block = jnp.dot(
            latent_rows, value_up_weight, preferred_element_type=jnp.float32
        ).astype(jnp.bfloat16)
        return (
            key_block.reshape(seg_rows, head_count, PLAIN_QK_DIM),
            value_block.reshape(seg_rows, head_count, VALUE_DIM),
            rope_block,
        )

    members = (
        lax.all_gather(ckv_all, "sp", axis=0, tiled=True),
        lax.all_gather(kr_all, "sp", axis=0, tiled=True),
    )
    block_count = members[0].shape[0] // seg_rows
    stacked = tuple(
        (member.reshape((block_count, seg_rows) + member.shape[1:]) for member in members)
    )

    def step_fn(state, key_group):
        key_block, value_block, rope_block = expand_latent(key_group)
        return (attend_block(state, key_block, value_block, rope_block), None)

    result, unused = lax.scan(step_fn, initial, stacked)
    running_max, running_sum, numerator = result
    attended = (
        (numerator / running_sum[..., None])
        .astype(jnp.bfloat16)
        .reshape(tok_count, head_count * VALUE_DIM)
    )
    proj_cols = jnp.dot(
        lax.all_gather(attended, "tp", axis=1, tiled=True),
        w_out,
        preferred_element_type=jnp.float32,
    )
    proj_rows = lax.all_to_all(
        proj_cols.astype(jnp.bfloat16), "tp", split_axis=0, concat_axis=1, tiled=True
    )
    mixed_rows = latents.astype(jnp.float32) + modulation[4] * proj_rows.astype(jnp.float32)
    return mixed_rows.astype(jnp.bfloat16)


MESH = pl.DeviceIdType.MESH
LOG2E = 1.4426950408889634
STEP = 16
BAND = 32


def turn_tables(tokens):
    freq_count = ROTARY_DIM // 4
    inverse = 10000.0 ** (-np.arange(freq_count) / freq_count)
    position = np.arange(tokens)
    cosine = np.zeros((tokens, 128), np.float32)
    sine = np.zeros((tokens, 128), np.float32)
    cosine[:, :PLAIN_QK_DIM] = 1.0
    for half_index, coordinate in enumerate((position // GRID_W, position % GRID_W)):
        angles = coordinate[:, None] * inverse[None, :]
        low = PLAIN_QK_DIM + 2 * half_index * freq_count
        high = low + freq_count
        cosine[:, low : low + freq_count] = np.cos(angles)
        cosine[:, high : high + freq_count] = np.cos(angles)
        sine[:, low : low + freq_count] = -np.sin(angles)
        sine[:, high : high + freq_count] = np.sin(angles)
    return cosine, sine


def lanes_of(shape):
    return lax.broadcasted_iota(jnp.int32, shape, len(shape) - 1)


def turned(values, cosine, sine):
    lane = lanes_of(values.shape)
    swapped = jnp.where(
        (lane // 8) % 2 == 0, pltpu.roll(values, 120, 1), pltpu.roll(values, 8, 1)
    )
    return values * cosine + swapped * sine


def block_kernel(
    cond_ref,
    bias_ref,
    qgain_ref,
    kvgain_ref,
    rope_ref,
    lat_hbm,
    ctx_hbm,
    wsh_hbm,
    wsc_hbm,
    wga_hbm,
    wqd_hbm,
    wkd_hbm,
    wqu_hbm,
    wku_hbm,
    wvu_hbm,
    wo_hbm,
    cos_hbm,
    sin_hbm,
    out_ref,
    cond16,
    w3,
    lat,
    ctx,
    hid,
    wqd,
    wkvr,
    modp,
    mod,
    cq,
    kv,
    kvc,
    kraw,
    ck,
    cqn,
    wqu,
    wku,
    wvu,
    wo,
    cosv,
    sinv,
    qh,
    kb,
    vb,
    acc,
    mx,
    att,
    po,
    pr,
    st_mean,
    st_rate,
    part,
    load_sem,
    send_sem,
    recv_sem,
    zsend,
    zrecv,
    dsend,
    drecv,
):
    f32, bf16 = jnp.float32, jnp.bfloat16
    spn = lax.axis_size("sp")
    p = lax.axis_index("tp")
    z = lax.axis_index("sp")
    core = lax.rem(p, 2)
    side = p // 2
    p1, p2, p3 = p ^ 1, p ^ 2, p ^ 3
    own = lat.shape[1]
    width = lat.shape[2]
    tok = own * 4
    pair = own * 2
    ctxn = ctx.shape[0]
    seg = tok + ctxn
    modw = w3.shape[2]
    heads = qh.shape[0]
    hrow = seg // 2
    qcols = cq.shape[3]
    kcols = kv.shape[3]
    krank = 4 * kcols

    loads = []

    def load(src, dst):
        copy = pltpu.make_async_copy(src, dst, load_sem.at[len(loads)])
        loads.append(copy)
        copy.start()
        return copy

    l_lat = load(lat_hbm, lat.at[p])
    l_w3 = [load(ref, w3.at[i]) for i, ref in enumerate((wsh_hbm, wsc_hbm, wga_hbm))]
    l_ctx = load(ctx_hbm, ctx)
    l_kd = load(wkd_hbm, wkvr.at[:, pl.ds(0, kcols)])
    l_qd = load(wqd_hbm, wqd)
    table_rows = pl.ds(pl.multiple_of(z * tok, 8), tok)
    l_cos = load(cos_hbm.at[table_rows], cosv)
    l_sin = load(sin_hbm.at[table_rows], sinv)
    l_ku = load(wku_hbm, wku)
    l_vu = load(wvu_hbm, wvu)
    l_qu = load(wqu_hbm, wqu)
    l_wo = load(wo_hbm, wo)

    barrier = pltpu.get_barrier_semaphore()
    for peer in (p1, p2, p3):
        pl.semaphore_signal(barrier, inc=1, device_id={"tp": peer}, device_id_type=MESH)
    for d in range(1, spn):
        pl.semaphore_signal(
            barrier, inc=1, device_id={"sp": lax.rem(z + d, spn)}, device_id_type=MESH
        )

    sends = []

    def remote(src, dst, index, target):
        return pltpu.make_async_remote_copy(
            src_ref=src,
            dst_ref=dst,
            send_sem=send_sem.at[index],
            recv_sem=recv_sem.at[index],
            device_id=target,
            device_id_type=MESH,
        )

    def send(src, dst, index, target):
        copy = remote(src, dst, index, target)
        copy.start()
        sends.append(copy)
        return copy

    counter = [0]

    def fresh():
        counter[0] += 1
        return counter[0] - 1

    def spread(view, far_view=None):
        far_view = far_view or view
        i1, i2, i3 = fresh(), fresh(), fresh()
        first = send(view(p), view(p), i2, {"tp": p2})
        second = send(view(p), view(p), i1, {"tp": p1})

        def relay():
            first.wait_recv()
            third = send(far_view(p2), far_view(p2), i3, {"tp": p1})
            return third.wait_recv

        return relay, second.wait_recv

    cond16[...] = jnp.zeros_like(cond16)
    cond16[0:2, :] = cond_ref[...]
    conditions = cond16[...]
    act = (conditions / (1.0 + jnp.exp(-conditions))).astype(bf16)

    pl.semaphore_wait(barrier, 3 + spn - 1)
    def near(view):
        return send(view(p), view(p), fresh(), {"tp": p1}).wait_recv

    def far(view):
        i2, i3 = fresh(), fresh()
        first = send(view(p), view(p), i2, {"tp": p2})

        def relay():
            first.wait_recv()
            return send(view(p2), view(p2), i3, {"tp": p1}).wait_recv

        return relay

    l_lat.wait()
    lat_near = near(lambda slot: lat.at[slot])
    lat_rows = [slice(r, r + BAND) for r in range(0, own, BAND)]
    lat_views = [lambda slot, r=r: lat.at[slot, pl.ds(r.start, BAND)] for r in lat_rows]
    lat_relay = [far(lat_views[0])]

    for i in range(3):
        l_w3[i].wait()
        partial_mod = jnp.dot(act, w3[i], preferred_element_type=f32)
        modp[z, 2 * i : 2 * i + 2, :] = partial_mod[0:2]
    modp[z, 6:8, :] = jnp.zeros((2, modw), f32)
    mod_waits = []
    for d in range(1, spn):
        mod_waits.append(
            send(modp.at[z], modp.at[z], fresh(), {"sp": lax.rem(z + d, spn)})
        )
    wkvr[:, kcols + ROTARY_DIM :] = jnp.zeros((width, wkvr.shape[1] - kcols - ROTARY_DIM), bf16)
    wkvr[:, kcols : kcols + ROTARY_DIM] = rope_ref[...]

    def measured(src, row_count, dst_row):
        @pl.loop(0, row_count // BAND)
        def _(i):
            rows = pl.ds(pl.multiple_of(i * BAND, BAND), BAND)
            to = pl.ds(pl.multiple_of(dst_row + i * BAND, BAND), BAND)
            tiles = [slice(c, c + 128) for c in range(0, width, 128)]
            sums = jnp.zeros((BAND, 128), f32)
            for c in tiles:
                sums = sums + src[rows, c].astype(f32)
            mean = jnp.broadcast_to(
                jnp.sum(sums, axis=-1, keepdims=True) * (1.0 / width), (BAND, 128)
            )
            squares = jnp.zeros((BAND, 128), f32)
            for c in tiles:
                center = src[rows, c].astype(f32) - mean
                squares = squares + center * center
            spread_of = jnp.sum(squares, axis=-1, keepdims=True) * (1.0 / width)
            st_mean[to, :] = mean
            st_rate[to, :] = jnp.broadcast_to(lax.rsqrt(spread_of + EPSILON), (BAND, 128))

    def modulate(src, row_count, dst_row, which):
        @pl.loop(0, row_count // BAND)
        def _(i):
            rows = pl.ds(pl.multiple_of(i * BAND, BAND), BAND)
            to = pl.ds(pl.multiple_of(dst_row + i * BAND, BAND), BAND)
            mean, rate = st_mean[to, :], st_rate[to, :]
            for c in range(0, width, 128):
                j, k = c // modw, c % modw
                shift_by = mod[j, which : which + 1, k : k + 128]
                scale_by = mod[j, 2 + which : 3 + which, k : k + 128]
                normed = (src[rows, c : c + 128].astype(f32) - mean) * rate
                hid[to, c : c + 128] = (normed * (1.0 + scale_by) + shift_by).astype(bf16)

    measured(lat.at[p], own, p * own)
    l_ctx.wait()
    measured(ctx, ctxn, tok)
    for copy in mod_waits:
        copy.wait_recv()
    total = modp[0]
    for i in range(1, spn):
        total = total + modp[i]
    mod[p] = total
    mod_waits = [send(mod.at[p], mod.at[p], fresh(), {"tp": peer}) for peer in (p2, p3, p1)]
    for view in lat_views[1:]:
        lat_relay.append(far(view))
    lat_near()
    measured(lat.at[p1], own, p1 * own)
    lat_far = [lat_relay[0]()]
    for copy in mod_waits:
        copy.wait_recv()

    modulate(ctx, ctxn, tok, 1)
    l_kd.wait()
    l_qd.wait()
    mixed_ctx = jnp.dot(hid[tok:, :], wkvr[...], preferred_element_type=f32)
    kvc[p] = mixed_ctx[:, :kcols].astype(bf16)
    kraw[tok:, :] = mixed_ctx[:, kcols:]
    relays = [spread(lambda slot: kvc.at[slot])]

    modulate(lat.at[p], own, p * own, 0)
    modulate(lat.at[p1], own, p1 * own, 0)

    def down(half):
        rows = pl.ds(pl.multiple_of(half * pair, STEP), pair)
        both = jnp.dot(hid[rows, :], wkvr[...], preferred_element_type=f32)
        kv[p, half] = both[:, :kcols].astype(bf16)
        kraw[rows, :] = both[:, kcols:]
        one = spread(lambda slot: kv.at[slot, half], lambda slot: kv.at[slot, 1 - half])
        cq[p, half] = jnp.dot(hid[rows, :], wqd[...], preferred_element_type=f32).astype(bf16)
        return one, spread(lambda slot: cq.at[slot, half], lambda slot: cq.at[slot, 1 - half])

    kv_a, cq_a = down(side)
    for n, r in enumerate(lat_rows):
        if n:
            lat_far.append(lat_relay[n]())
        piece = lat.at[p2, pl.ds(r.start, BAND)]
        measured(piece, BAND, p2 * own + r.start)
        modulate(piece, BAND, p2 * own + r.start, 0)
    for n, r in enumerate(lat_rows):
        lat_far[n]()
        piece = lat.at[p3, pl.ds(r.start, BAND)]
        measured(piece, BAND, p3 * own + r.start)
        modulate(piece, BAND, p3 * own + r.start, 0)
    kv_b, cq_b = down(1 - side)
    relays += [kv_a, kv_b]
    kv_far = [r() for r, _ in relays]
    for w in kv_far:
        w()
    for _, w in relays:
        w()

    l_cos.wait()
    l_sin.wait()
    kr_lat = turned(pltpu.roll(kraw[:tok, :], 64, 1), cosv[...], sinv[...])
    kraw[:tok, :] = kr_lat
    kraw[tok:, :] = pltpu.roll(kraw[tok:, :], 64, 1)
    for hf in range(2):
        for t in range(4):
            packed = None
            for j in range(4):
                first_row = hf * hrow + (4 * t + j) * STEP
                moved = pltpu.roll(
                    kraw[first_row : first_row + STEP, :], (32 * j + 64) % 128, 1
                )
                packed = moved if packed is None else packed + moved
            ck[z, hf, hrow : hrow + STEP, 128 * t : 128 * t + 128] = packed.astype(bf16)

    def rms(pieces, gain_ref, store):
        values = [piece.astype(f32) for piece in pieces]
        total_of = None
        for v in values:
            s = jnp.sum(v * v, axis=-1, keepdims=True)
            total_of = s if total_of is None else total_of + s
        cols = values[0].shape[1]
        factor = lax.rsqrt(total_of / (cols * len(values)) + EPSILON)
        for j, v in enumerate(values):
            gain = gain_ref[0:1, j * cols : (j + 1) * cols]
            store(slice(j * cols, (j + 1) * cols), (v * factor * gain).astype(bf16))

    for piece in range(seg // 64):
        base = piece * 64
        if base < tok:
            chunk = [kv[r, base // pair, base % pair : base % pair + 64, :] for r in range(4)]
        else:
            chunk = [kvc[r, base - tok : base - tok + 64, :] for r in range(4)]

        def put(cols, value, base=base):
            ck[z, base // hrow, base % hrow : base % hrow + 64, cols] = value

        rms(chunk, kvgain_ref, put)

    def hop(origin, target, way):
        return pltpu.make_async_remote_copy(
            src_ref=ck.at[origin, core],
            dst_ref=ck.at[origin, core],
            send_sem=zsend.at[way, origin],
            recv_sem=zrecv.at[origin],
            device_id={"sp": target},
            device_id_type=MESH,
        )

    def cross(origin, half):
        return pltpu.make_async_remote_copy(
            src_ref=ck.at[origin, half],
            dst_ref=ck.at[origin, half],
            send_sem=dsend.at[origin],
            recv_sem=drecv.at[origin],
            device_id={"tp": p1},
            device_id_type=MESH,
        )

    has_right = z + 1 < spn
    has_left = z >= 1

    @pl.when(has_right)
    def _():
        hop(z, z + 1, 0).start()

    @pl.when(has_left)
    def _():
        hop(z, z - 1, 1).start()

    w_cq = [cq_a[0](), cq_b[0]()]
    for w in w_cq:
        w()
    cq_a[1]()
    cq_b[1]()
    for piece in range(tok // 64):
        base = piece * 64
        chunk = [cq[r, base // pair, base % pair : base % pair + 64, :] for r in range(4)]

        def put(cols, value, base=base):
            cqn[base : base + 64, cols] = value

        rms(chunk, qgain_ref, put)
    l_qu.wait()
    q_all = jnp.dot(cqn[...], wqu[...], preferred_element_type=f32)
    lane = lanes_of((tok, 128))
    for h in range(heads):
        offset = h * (PLAIN_QK_DIM + ROTARY_DIM)
        tile, shift = offset // 128, offset % 128
        head = q_all[:, 128 * tile : 128 * tile + 128]
        if shift:
            head = pltpu.roll(head, 128 - shift, 1)
            if shift + PLAIN_QK_DIM + ROTARY_DIM > 128:
                rest = pltpu.roll(q_all[:, 128 * tile + 128 : 128 * tile + 256], 128 - shift, 1)
                head = jnp.where(lane < 128 - shift, head, rest)
        qh[h] = turned(head, cosv[...], sinv[...]).astype(bf16)
    l_ku.wait()
    l_vu.wait()
    acc[...] = jnp.zeros_like(acc)
    mx[...] = jnp.full(mx.shape, NEGATIVE, f32)
    factor = (PLAIN_QK_DIM + ROTARY_DIM) ** (-0.5) * LOG2E

    def arrive(step):
        left, right = z - 1 - step, z + 1 + step

        @pl.when(left >= 0)
        def _():
            hop(left, z, 0).wait_recv()
            cross(left, core).start()

            @pl.when(has_right)
            def _():
                hop(left, z + 1, 0).start()

        @pl.when(right < spn)
        def _():
            hop(right, z, 1).wait_recv()
            cross(right, core).start()

            @pl.when(has_left)
            def _():
                hop(right, z - 1, 1).start()

    def expand(block):
        lane_h = lanes_of((hrow, 128))
        ones = (lane_h == VALUE_DIM).astype(f32)
        lane_s = lanes_of((STEP, 128))
        on_rope = (lane_s >= PLAIN_QK_DIM) & (lane_s < PLAIN_QK_DIM + ROTARY_DIM)
        for hf in range(2):
            rows = slice(hf * hrow, (hf + 1) * hrow)
            latent_rows = ck[block, hf, :hrow, :]
            pieces = []
            for t in range(4):
                packed = ck[block, hf, hrow : hrow + STEP, 128 * t : 128 * t + 128].astype(f32)
                for j in range(4):
                    moved = pltpu.roll(packed, (192 - 32 * j) % 128, 1)
                    pieces.append(jnp.where(on_rope, moved, 0.0))
            rope_key = jnp.concatenate(pieces, axis=0)
            keys = jnp.dot(latent_rows, wku[...], preferred_element_type=f32)
            vals = jnp.dot(latent_rows, wvu[...], preferred_element_type=f32)
            for hp in range(heads // 2):
                cols = slice(128 * hp, 128 * hp + 128)
                k2, v2 = keys[:, cols], vals[:, cols]
                kb[2 * hp, rows, :] = jnp.where(lane_h < 64, k2, rope_key).astype(bf16)
                kb[2 * hp + 1, rows, :] = jnp.where(
                    lane_h < 64, pltpu.roll(k2, 64, 1), rope_key
                ).astype(bf16)
                vb[2 * hp, rows, :] = jnp.where(lane_h < 64, v2, ones).astype(bf16)
                vb[2 * hp + 1, rows, :] = jnp.where(
                    lane_h < 64, pltpu.roll(v2, 64, 1), ones
                ).astype(bf16)

    def score(h):
        return lax.dot_general(
            qh[h], kb[h], (((1,), (1,)), ((), ())), preferred_element_type=f32
        )

    def attend(h, scores):
        tiles = [scores[:, c : c + 128] * factor for c in range(0, seg, 128)]
        bias = bias_ref[h] * LOG2E
        tiles = [t + bias if n * 128 >= tok else t for n, t in enumerate(tiles)]
        best = functools.reduce(jnp.maximum, tiles)
        old = mx[h]
        new = jnp.maximum(old, jnp.max(best, axis=-1, keepdims=True))
        mx[h] = new
        weights = jnp.concatenate([jnp.exp2(t - new).astype(bf16) for t in tiles], axis=1)
        acc[h] = acc[h] * jnp.exp2(old - new) + jnp.dot(
            weights, vb[h], preferred_element_type=f32
        )

    def attend_all(after):
        scores = score(0)
        for h in range(heads):
            following = score(h + 1) if h + 1 < heads else None
            attend(h, scores)
            after(h)
            scores = following

    def block_at(step):
        below = jnp.minimum(z, spn - 1 - z)
        near = jnp.where(lax.rem(step, 2) == 1, z - (step + 1) // 2, z + step // 2)
        past = jnp.where(z < spn - 1 - z, step, spn - 1 - step)
        return jnp.where(step <= 2 * below, near, past)

    @pl.loop(0, spn - 1)
    def _(step):
        @pl.when(step > 0)
        def _():
            arrive(step - 1)

        block = block_at(step)

        @pl.when(step > 0)
        def _():
            cross(block, 1 - core).wait_recv()

        expand(block)
        attend_all(lambda h: None)

    att_relay, att_near = [], []
    lane64 = lane < 64

    def finish(h):
        if h % 2 == 0:
            return
        hp = h // 2
        outs = []
        for g in (h - 1, h):
            a = acc[g]
            outs.append(a / a[:, VALUE_DIM : VALUE_DIM + 1])
        att[p, hp] = jnp.where(lane64, outs[0], pltpu.roll(outs[1], 64, 1)).astype(bf16)
        att_relay.append(far(lambda slot: att.at[slot, hp]))
        att_near.append(near(lambda slot: att.at[slot, hp]))

    arrive(spn - 2)
    last_block = block_at(jnp.int32(spn - 1))
    cross(last_block, 1 - core).wait_recv()
    expand(last_block)
    attend_all(finish)

    l_wo.wait()
    half_k = heads * VALUE_DIM * 2
    order = (p2, p3, p1, p)

    def project(dest, chip):
        rows = pl.ds(pl.multiple_of(dest * own, STEP), own)
        joined = jnp.concatenate(
            [att[2 * chip + r, hp, rows, :] for r in range(2) for hp in range(heads // 2)], axis=1
        )
        k_rows = pl.ds(pl.multiple_of(chip * half_k, 128), half_k)
        return jnp.dot(joined, wo[k_rows, :], preferred_element_type=f32)

    att_far = [att_relay[0](), att_relay[1]()]
    for w in att_near:
        w()
    for dest in order:
        part[dest] = project(dest, side)
    att_far += [r() for r in att_relay[2:]]
    for w in att_far:
        w()
    final = []
    for dest in order:
        made = (part[dest] + project(dest, 1 - side)).astype(bf16)
        if dest is p:
            pr[p] = made
        else:
            po[dest] = made
            final.append(send(po.at[dest], pr.at[p], fresh(), {"tp": dest}))
    for copy in final:
        copy.wait_recv()

    @pl.loop(0, own // STEP)
    def _(i):
        rows = pl.ds(pl.multiple_of(i * STEP, STEP), STEP)
        for j in range(4):
            cols = slice(j * modw, (j + 1) * modw)
            gate = mod[j, 4:5, :]
            out_ref[rows, cols] = (
                lat[p, rows, cols].astype(f32) + gate * pr[j, rows, :].astype(f32)
            ).astype(bf16)

    for copy in sends:
        copy.wait_send()

    @pl.when(has_right)
    def _():
        hop(z, z + 1, 0).wait_send()

    @pl.when(has_left)
    def _():
        hop(z, z - 1, 1).wait_send()

    for step in range(spn - 1):
        left, right = z - 1 - step, z + 1 + step

        @pl.when(left >= 0)
        def _():
            cross(left, core).wait_send()

            @pl.when(has_right)
            def _():
                hop(left, z + 1, 0).wait_send()

        @pl.when(right < spn)
        def _():
            cross(right, core).wait_send()

            @pl.when(has_left)
            def _():
                hop(right, z - 1, 1).wait_send()


def fused_device(
    latents,
    conditions,
    context,
    w_shift,
    w_scale,
    w_gate,
    w_qdown,
    w_kvdown,
    w_rope,
    q_gain,
    latent_norm_gain,
    query_up_weight,
    key_up_weight,
    value_up_weight,
    context_bias,
    w_out,
):
    f32, bf16 = jnp.float32, jnp.bfloat16
    spn = lax.axis_size("sp")
    own, width = latents.shape
    ctxn = context.shape[0]
    tok = 4 * own
    seg = tok + ctxn
    heads = context_bias.shape[0]
    modw = w_shift.shape[1]
    kdim, qcols = w_qdown.shape
    kcols = w_kvdown.shape[1]
    cosine, sine = turn_tables(tok * spn)
    vmem = pl.BlockSpec(memory_space=pltpu.VMEM)
    smem = pl.BlockSpec(memory_space=pltpu.SMEM)
    hbm = pl.BlockSpec(memory_space=pl.ANY)
    V, DMA = pltpu.VMEM, pltpu.SemaphoreType.DMA
    scratch = [
        V((16, conditions.shape[1]), f32),
        V((3,) + w_shift.shape, bf16),
        V((4, own, width), bf16),
        V((ctxn, width), bf16),
        V((seg, width), bf16),
        V((kdim, qcols), bf16),
        V((kdim, kcols + 128), bf16),
        V((spn, 8, modw), f32),
        V((4, 8, modw), f32),
        V((4, 2, 2 * own, qcols), bf16),
        V((4, 2, 2 * own, kcols), bf16),
        V((4, ctxn, kcols), bf16),
        V((seg, 128), f32),
        V((spn, 2, seg // 2 + STEP, 4 * kcols), bf16),
        V((tok, 4 * qcols), bf16),
        V(query_up_weight.shape, bf16),
        V(key_up_weight.shape, bf16),
        V(value_up_weight.shape, bf16),
        V(w_out.shape, bf16),
        V((tok, 128), f32),
        V((tok, 128), f32),
        V((heads, tok, 128), bf16),
        V((heads, seg, 128), bf16),
        V((heads, seg, 128), bf16),
        V((heads, tok, 128), f32),
        V((heads, tok, 128), f32),
        V((4, heads // 2, tok, 128), bf16),
        V((4, own, modw), bf16),
        V((4, own, modw), bf16),
        V((seg, 128), f32),
        V((seg, 128), f32),
        V((4, own, modw), f32),
        DMA((13,)),
        DMA((48,)),
        DMA((48,)),
        DMA((2, spn)),
        DMA((spn,)),
        DMA((spn,)),
        DMA((spn,)),
    ]
    return pl.pallas_call(
        block_kernel,
        out_shape=jax.ShapeDtypeStruct(latents.shape, bf16),
        in_specs=[vmem, smem, vmem, vmem, vmem] + [hbm] * 13,
        out_specs=vmem,
        scratch_shapes=scratch,
        compiler_params=pltpu.CompilerParams(
            collective_id=0, has_side_effects=True, vmem_limit_bytes=60 * 1024 * 1024
        ),
    )(
        conditions,
        context_bias,
        q_gain[None, :],
        latent_norm_gain[None, :],
        w_rope,
        latents,
        context,
        w_shift,
        w_scale,
        w_gate,
        w_qdown,
        w_kvdown,
        query_up_weight,
        key_up_weight,
        value_up_weight,
        w_out,
        jnp.asarray(cosine),
        jnp.asarray(sine),
    )


def on_device(*arrays):
    latents, context, bias = arrays[0], arrays[2], arrays[14]
    fits = (
        lax.axis_size("tp") == 4
        and latents.shape[0] % 32 == 0
        and context.shape[0] % 64 == 0
        and (4 * latents.shape[0] + context.shape[0]) == 512
        and arrays[6].shape[1] == 256
        and arrays[7].shape[1] == 128
        and bias.shape[0] == 8
    )
    return fused_device(*arrays) if fits else plain_device(*arrays)


def solution(mesh):
    in_specs = (
        P(("grp", "sp", "tp"), None),
        P("grp", "sp"),
        P(("grp", "sp"), None),
        P("sp", "tp"),
        P("sp", "tp"),
        P("sp", "tp"),
        P(None, "tp"),
        P(None, "tp"),
        P(),
        P(),
        P(),
        P(None, "tp"),
        P(None, "tp"),
        P(None, "tp"),
        P("tp"),
        P(None, "tp"),
    )
    out_specs = P(("grp", "sp", "tp"), None)
    return jax.shard_map(
        on_device, mesh=mesh, in_specs=in_specs, out_specs=out_specs, check_vma=False
    )
```
